32 devices in a mesh: fs: 8 (over z, y), tp: 4 (over x, core).
Axes of the slice: x: 2, y: 2, z: 4, core: 2. Of those that a mesh axis runs over, the one named last changes fastest.
Arguments:
- block_input: bfloat16 [1536, 2048], P('fs'), may hold values from -6 to 6
- query_cotangent: bfloat16 [1536, 1024], P('fs', 'tp'), may hold values from -0.15625 to 0.15625
- key_cotangent: bfloat16 [1536, 1024], P('fs', 'tp'), may hold values from -0.15625 to 0.15625
- query_factor: bfloat16 [2048, 256], P('fs'), may hold values from -0.125 to 0.125
- key_factor: bfloat16 [2048, 256], P('fs'), may hold values from -0.125 to 0.125
- query_first: float32 [256, 1024], P('fs', 'tp'), may hold values from -0.6 to 0.6
- query_second: float32 [256, 1024], P('fs', 'tp'), may hold values from 0.005 to 0.03
- key_first: float32 [256, 1024], P('fs', 'tp'), may hold values from -0.6 to 0.6
- key_second: float32 [256, 1024], P('fs', 'tp'), may hold values from 0.005 to 0.03
- query_weight: float32 [2048, 1024], P('fs', 'tp'), may hold values from -0.125 to 0.125
- key_weight: float32 [2048, 1024], P('fs', 'tp'), may hold values from -0.125 to 0.125
Outputs:
- query_update: float32 [2048, 1024], P('fs', 'tp')
- query_new: float32 [2048, 1024], P('fs', 'tp')
- query_copy: bfloat16 [2048, 1024], P(None, 'tp')
- query_first_new: float32 [256, 1024], P('fs', 'tp')
- query_second_new: float32 [256, 1024], P('fs', 'tp')
- key_update: float32 [2048, 1024], P('fs', 'tp')
- key_new: float32 [2048, 1024], P('fs', 'tp')
- key_copy: bfloat16 [2048, 1024], P(None, 'tp')
- key_first_new: float32 [256, 1024], P('fs', 'tp')
- key_second_new: float32 [256, 1024], P('fs', 'tp')
The draws below stay inside these ranges and needn't reach their ends.
All inputs are finite; a program needn't handle non-finite values.
Results may differ from the reference program's by a relative error of at most 0.0005.
Values may be sent and summed in bfloat16 or wider, within the bound.
No kernel may reach another device: no remote copies, remote signals or barrier semaphores. Data moves between devices by JAX's collectives and lax.ppermute only.
A program may use at most 64 MiB of HBM per device.

```python
import math
import jax
import jax.numpy as jnp
from jax import lax

D = 2048
WIDTH = 1024
RANK = 256
TOKENS = 1536


def block_levels(own_key, extent, split, smallest, high):
    def one(axis_at, shards_of):
        steps = jax.random.uniform(jax.random.fold_in(jax.random.fold_in(own_key, 6), axis_at), (shards_of,), jnp.float32, smallest / len(split), high / len(split))
        return jnp.repeat(jnp.exp(steps), extent[axis_at] // shards_of).reshape((-1,) + (1,) * (len(extent) - axis_at - 1))

    loudness = one(*split[0])
    for cut in split[1:]:
        loudness = loudness * one(*cut)
    return loudness


def gaussian(stream_key, shape, width, limit, pieces=(), kind=jnp.bfloat16):
    factor_of = block_levels(stream_key, shape, pieces, -0.22, 0.18) if pieces else 1.0
    array = jax.random.normal(stream_key, shape, jnp.float32) * width * factor_of
    return jnp.minimum(jnp.maximum(array, -limit), limit).astype(kind)


def setup_inputs(seed: int = 0) -> dict:
    keys = jax.random.split(jax.random.key(seed), 12)
    return {
        "block_input": gaussian(keys[0], (TOKENS, D), 1.0, 6.0, ((0, 8),)),
        "query_cotangent": gaussian(keys[1], (TOKENS, WIDTH), TOKENS ** -0.5, 0.15625, ((0, 8), (1, 4))),
        "key_cotangent": gaussian(keys[2], (TOKENS, WIDTH), TOKENS ** -0.5, 0.15625, ((0, 8), (1, 4))),
        "query_factor": gaussian(keys[3], (D, RANK), D ** -0.5, 0.125, ((0, 8),)),
        "key_factor": gaussian(keys[4], (D, RANK), D ** -0.5, 0.125, ((0, 8),)),
        "query_first": gaussian(keys[5], (RANK, WIDTH), 0.1, 0.6, ((0, 8), (1, 4)), jnp.float32),
        "query_second": jnp.clip(jnp.exp(math.log(0.03) - 1.7917595 * jax.random.uniform(keys[6], (RANK, WIDTH), jnp.float32) ** block_levels(keys[6], (RANK, WIDTH), ((0, 8), (1, 4)), -0.2, 0.2)), 0.005, 0.03),
        "key_first": gaussian(keys[7], (RANK, WIDTH), 0.1, 0.6, ((0, 8), (1, 4)), jnp.float32),
        "key_second": jnp.clip(jnp.exp(math.log(0.03) - 1.7917595 * jax.random.uniform(keys[8], (RANK, WIDTH), jnp.float32) ** block_levels(keys[8], (RANK, WIDTH), ((0, 8), (1, 4)), -0.2, 0.2)), 0.005, 0.03),
        "query_weight": gaussian(keys[9], (D, WIDTH), D ** -0.5, 0.125, ((0, 8), (1, 4)), jnp.float32),
        "key_weight": gaussian(keys[10], (D, WIDTH), D ** -0.5, 0.125, ((0, 8), (1, 4)), jnp.float32),
    }


beta_one = 0.9
beta_two = 0.99
denom_floor = 0.001
scale_floor = 0.5
learn_rate = 0.02

def one_update(block_input, cotangent, factor, first, second, weight):
    gradient = jnp.dot(block_input.T, cotangent, preferred_element_type=jnp.float32)
    factor_wide = factor.astype(jnp.float32)
    small = jnp.dot(factor_wide.T, gradient, precision=lax.Precision.HIGHEST)
    first_new = beta_one * first + (1.0 - beta_one) * small
    second_new = beta_two * second + (1.0 - beta_two) * small * small
    direction = first_new / (jnp.sqrt(second_new) + denom_floor)
    spread = jnp.sqrt(jnp.sum(direction * direction) / direction.size)
    scale = 1.0 / jnp.maximum(spread, scale_floor)
    update = -scale * jnp.dot(factor_wide, direction, precision=lax.Precision.HIGHEST)
    fresh = weight + learn_rate * update
    return (update, fresh, fresh.astype(jnp.bfloat16), first_new, second_new)

def reference(block_input, query_cotangent, key_cotangent, query_factor, key_factor, query_first, query_second, key_first, key_second, query_weight, key_weight):
    query_out = one_update(block_input, query_cotangent, query_factor, query_first, query_second, query_weight)
    key_out = one_update(block_input, key_cotangent, key_factor, key_first, key_second, key_weight)
    return (query_out[0], query_out[1], query_out[2], query_out[3], query_out[4], key_out[0], key_out[1], key_out[2], key_out[3], key_out[4])
```

```python
import jax
import jax.numpy as jnp
from jax import lax
from jax.sharding import PartitionSpec as P

beta_one = 0.9
beta_two = 0.99
denom_floor = 0.001
scale_floor = 0.5
learn_rate = 0.02


def moments(small, first, second):
    first_new = beta_one * first + (1.0 - beta_one) * small
    second_new = beta_two * second + (1.0 - beta_two) * small * small
    direction = first_new / (jnp.sqrt(second_new) + denom_floor)
    return (first_new, second_new, direction)


def split_three(values):
    upper = lax.optimization_barrier(values.astype(jnp.bfloat16))
    rest = values - upper.astype(jnp.float32)
    middle = lax.optimization_barrier(rest.astype(jnp.bfloat16))
    lower = (rest - middle.astype(jnp.float32)).astype(jnp.bfloat16)
    return (upper, middle, lower)


def project_tokens(mixed, cotangent):
    contract = (((0,), (0,)), ((), ()))
    total = jnp.zeros((mixed.shape[1], cotangent.shape[1]), jnp.float32)
    for piece in split_three(mixed):
        total = total + lax.dot_general(
            piece, cotangent, contract, preferred_element_type=jnp.float32
        )
    return total


def apply_factor(factor, direction):
    total = jnp.zeros((factor.shape[0], direction.shape[1]), jnp.float32)
    for piece in split_three(direction):
        total = total + jnp.dot(factor, piece, preferred_element_type=jnp.float32)
    return total


def relayed(block):
    count = lax.axis_size("fs")
    blocks = {0: block}
    for offset in sorted(range(1, count), key=lambda k: (bin(k).count("1"), -(k & -k))):
        step = offset & -offset
        blocks[offset] = lax.ppermute(
            blocks[offset ^ step], "fs", [(i, i ^ step) for i in range(count)]
        )
    return blocks


def few_devices():
    count = lax.axis_size("fs")
    return count <= 16 and count & (count - 1) == 0


def mix(block_input, factors):
    if not few_devices():
        whole = lax.all_gather(factors, "fs", axis=0, tiled=True)
        return jnp.dot(block_input, whole, preferred_element_type=jnp.float32)
    rows = factors.shape[0]
    own = lax.axis_index("fs")
    total = None
    for offset, block in relayed(factors).items():
        columns = lax.dynamic_slice_in_dim(block_input, (own ^ offset) * rows, rows, 1)
        part = jnp.dot(columns, block, preferred_element_type=jnp.float32)
        total = part if total is None else total + part
    return total


def gather_copies(query_new, key_new):
    query_own = query_new.astype(jnp.bfloat16)
    key_own = key_new.astype(jnp.bfloat16)
    if not few_devices():
        return (
            lax.all_gather(query_own, "fs", axis=0, tiled=True),
            lax.all_gather(key_own, "fs", axis=0, tiled=True),
        )
    rows, columns = query_own.shape
    own = lax.axis_index("fs")
    query_copy = jnp.zeros((rows * lax.axis_size("fs"), columns), jnp.bfloat16)
    key_copy = jnp.zeros((rows * lax.axis_size("fs"), columns), jnp.bfloat16)
    for offset, block in relayed(jnp.stack((query_own, key_own))).items():
        start = (own ^ offset) * rows
        query_copy = lax.dynamic_update_slice(query_copy, block[0], (start, 0))
        key_copy = lax.dynamic_update_slice(key_copy, block[1], (start, 0))
    return (query_copy, key_copy)


def sum_over(values, axis):
    count = lax.axis_size(axis)
    total = values
    for shift in range(1, count):
        total = total + lax.ppermute(
            values, axis, [(i, (i + shift) % count) for i in range(count)]
        )
    return total


def body(
    block_input,
    query_cotangent,
    key_cotangent,
    query_factor,
    key_factor,
    query_first,
    query_second,
    key_first,
    key_second,
    query_weight,
    key_weight,
):
    count = lax.axis_size("fs")
    rank = query_factor.shape[1]
    columns = query_cotangent.shape[1]
    mixed = mix(block_input, jnp.concatenate((query_factor, key_factor), axis=1))
    query_part = project_tokens(mixed[:, :rank], query_cotangent)
    key_part = project_tokens(mixed[:, rank:], key_cotangent)
    parts = jnp.stack(
        (
            query_part.reshape(count, rank // count, columns),
            key_part.reshape(count, rank // count, columns),
        ),
        axis=1,
    )
    small = jnp.sum(lax.all_to_all(parts, "fs", 0, 0, tiled=True), axis=0)
    query_first_new, query_second_new, query_direction = moments(
        small[0], query_first, query_second
    )
    key_first_new, key_second_new, key_direction = moments(small[1], key_first, key_second)
    own_directions = jnp.stack((query_direction, key_direction))
    directions = lax.all_to_all(
        jnp.broadcast_to(own_directions[None], (count,) + own_directions.shape),
        "fs",
        0,
        0,
        tiled=True,
    )
    full_query = directions[:, 0].reshape(rank, columns)
    full_key = directions[:, 1].reshape(rank, columns)
    squares = jnp.stack((jnp.sum(full_query * full_query), jnp.sum(full_key * full_key)))
    squares = sum_over(jnp.broadcast_to(squares[:, None], (2, 128)), "tp")[:, :1]
    entry_count = rank * columns * lax.axis_size("tp")
    scales = 1.0 / jnp.maximum(jnp.sqrt(squares / entry_count), scale_floor)
    query_update = -scales[0] * apply_factor(query_factor, full_query)
    key_update = -scales[1] * apply_factor(key_factor, full_key)
    query_new = query_weight + learn_rate * query_update
    key_new = key_weight + learn_rate * key_update
    query_copy, key_copy = gather_copies(query_new, key_new)
    return (
        query_update,
        query_new,
        query_copy,
        query_first_new,
        query_second_new,
        key_update,
        key_new,
        key_copy,
        key_first_new,
        key_second_new,
    )


def solution(mesh):
    in_specs = (
        P("fs", None),
        P("fs", "tp"),
        P("fs", "tp"),
        P("fs", None),
        P("fs", None),
        P("fs", "tp"),
        P("fs", "tp"),
        P("fs", "tp"),
        P("fs", "tp"),
        P("fs", "tp"),
        P("fs", "tp"),
    )
    out_specs = (
        P("fs", "tp"),
        P("fs", "tp"),
        P(None, "tp"),
        P("fs", "tp"),
        P("fs", "tp"),
        P("fs", "tp"),
        P("fs", "tp"),
        P(None, "tp"),
        P("fs", "tp"),
        P("fs", "tp"),
    )
    return jax.shard_map(body, mesh=mesh, in_specs=in_specs, out_specs=out_specs, check_vma=False)
```

```python
import jax
import jax.numpy as jnp
from jax import lax
from jax.experimental import pallas as pl
from jax.experimental.pallas import tpu as pltpu
from jax.sharding import PartitionSpec as P

beta_one = 0.9
beta_two = 0.99
denom_floor = 0.001
scale_floor = 0.5
learn_rate = 0.02


def moments(small, first, second):
    first_new = beta_one * first + (1.0 - beta_one) * small
    second_new = beta_two * second + (1.0 - beta_two) * small * small
    direction = first_new / (jnp.sqrt(second_new) + denom_floor)
    return (first_new, second_new, direction)


def split_three(values):
    upper = lax.optimization_barrier(values.astype(jnp.bfloat16))
    rest = values - upper.astype(jnp.float32)
    middle = lax.optimization_barrier(rest.astype(jnp.bfloat16))
    lower = (rest - middle.astype(jnp.float32)).astype(jnp.bfloat16)
    return (upper, middle, lower)


def project_tokens(mixed, cotangent):
    contract = (((0,), (0,)), ((), ()))
    total = jnp.zeros((mixed.shape[1], cotangent.shape[1]), jnp.float32)
    for piece in split_three(mixed):
        total = total + lax.dot_general(
            piece, cotangent, contract, preferred_element_type=jnp.float32
        )
    return total


def apply_factor(factor, direction):
    total = jnp.zeros((factor.shape[0], direction.shape[1]), jnp.float32)
    for piece in split_three(direction):
        total = total + jnp.dot(factor, piece, preferred_element_type=jnp.float32)
    return total


def relayed(block):
    count = lax.axis_size("fs")
    blocks = {0: block}
    for offset in sorted(range(1, count), key=lambda k: (bin(k).count("1"), -(k & -k))):
        step = offset & -offset
        blocks[offset] = lax.ppermute(
            blocks[offset ^ step], "fs", [(i, i ^ step) for i in range(count)]
        )
    return blocks


def few_devices():
    count = lax.axis_size("fs")
    return count <= 16 and count & (count - 1) == 0


def mix(block_input, factors):
    if not few_devices():
        whole = lax.all_gather(factors, "fs", axis=0, tiled=True)
        return jnp.dot(block_input, whole, preferred_element_type=jnp.float32)
    rows = factors.shape[0]
    own = lax.axis_index("fs")
    total = None
    blocks = relayed(factors)
    for offset, block in blocks.items():
        columns = lax.dynamic_slice_in_dim(block_input, (own ^ offset) * rows, rows, 1)
        part = jnp.dot(columns, block, preferred_element_type=jnp.float32)
        total = part if total is None else total + part
    return total


def place_blocks(blocks, own):
    count = len(blocks)
    rows, columns = blocks[0].shape[1:]

    def kernel(own_ref, *refs):
        outs = refs[count : count + 2]
        staged, left, stage = refs[count + 3], refs[count + 2], refs[count + 4]
        loads = []
        stores = []
        for offset in range(count):
            loads.append(
                pltpu.make_async_copy(refs[offset], stage.at[offset], staged.at[offset])
            )
            start = pl.multiple_of((own_ref[0] ^ offset) * rows, rows)
            for which in range(2):
                stores.append(
                    pltpu.make_async_copy(
                        stage.at[offset, which],
                        outs[which].at[pl.ds(start, rows)],
                        left.at[2 * offset + which],
                    )
                )
        for load in loads:
            load.start()
        for offset in range(count):
            loads[offset].wait()
            stores[2 * offset].start()
            stores[2 * offset + 1].start()
        for store in stores:
            store.wait()

    out = jax.ShapeDtypeStruct((rows * count, columns), blocks[0].dtype)
    anywhere = pl.BlockSpec(memory_space=pl.ANY)
    return pl.pallas_call(
        kernel,
        in_specs=[pl.BlockSpec(memory_space=pltpu.SMEM)] + [anywhere] * count,
        out_specs=(anywhere, anywhere),
        out_shape=(out, out),
        scratch_shapes=[
            pltpu.SemaphoreType.DMA((2 * count,)),
            pltpu.SemaphoreType.DMA((count,)),
            pltpu.VMEM((count, 2, rows, columns), blocks[0].dtype),
        ],
    )(own.reshape(1).astype(jnp.int32), *(blocks[offset] for offset in range(count)))


def gather_copies(query_new, key_new):
    query_own = query_new.astype(jnp.bfloat16)
    key_own = key_new.astype(jnp.bfloat16)
    if not few_devices():
        return (
            lax.all_gather(query_own, "fs", axis=0, tiled=True),
            lax.all_gather(key_own, "fs", axis=0, tiled=True),
        )
    blocks = relayed(jnp.stack((query_own, key_own)))
    return tuple(place_blocks(blocks, lax.axis_index("fs")))


def sum_over(values, axis):
    count = lax.axis_size(axis)
    total = values
    for shift in range(1, count):
        total = total + lax.ppermute(
            values, axis, [(i, (i + shift) % count) for i in range(count)]
        )
    return total


def body(
    block_input,
    query_cotangent,
    key_cotangent,
    query_factor,
    key_factor,
    query_first,
    query_second,
    key_first,
    key_second,
    query_weight,
    key_weight,
):
    count = lax.axis_size("fs")
    rank = query_factor.shape[1]
    columns = query_cotangent.shape[1]
    pairs = lax.axis_size("tp")
    even = lax.axis_index("tp") % 2 == 0
    near = mix(block_input, jnp.where(even, query_factor, key_factor))
    far = lax.ppermute(near, "tp", [(i, i ^ 1) for i in range(pairs)])
    near_part = project_tokens(near, jnp.where(even, query_cotangent, key_cotangent))
    far_part = project_tokens(far, jnp.where(even, key_cotangent, query_cotangent))
    parts = jnp.stack(
        (
            near_part.reshape(count, rank // count, columns),
            far_part.reshape(count, rank // count, columns),
        ),
        axis=1,
    )
    small = jnp.sum(lax.all_to_all(parts, "fs", 0, 0, tiled=True), axis=0)
    small_query = jnp.where(even, small[0], small[1])
    small_key = jnp.where(even, small[1], small[0])
    query_first_new, query_second_new, query_direction = moments(
        small_query, query_first, query_second
    )
    key_first_new, key_second_new, key_direction = moments(small_key, key_first, key_second)
    own_directions = jnp.stack((query_direction, key_direction))
    directions = lax.all_to_all(
        jnp.broadcast_to(own_directions[None], (count,) + own_directions.shape),
        "fs",
        0,
        0,
        tiled=True,
    )
    full_query = directions[:, 0].reshape(rank, columns)
    full_key = directions[:, 1].reshape(rank, columns)
    squares = jnp.stack((jnp.sum(full_query * full_query), jnp.sum(full_key * full_key)))
    squares = sum_over(jnp.broadcast_to(squares[:, None], (2, 128)), "tp")[:, :1]
    entry_count = rank * columns * lax.axis_size("tp")
    scales = 1.0 / jnp.maximum(jnp.sqrt(squares / entry_count), scale_floor)
    query_update = -scales[0] * apply_factor(query_factor, full_query)
    key_update = -scales[1] * apply_factor(key_factor, full_key)
    query_new = query_weight + learn_rate * query_update
    key_new = key_weight + learn_rate * key_update
    query_copy, key_copy = gather_copies(query_new, key_new)
    return (
        query_update,
        query_new,
        query_copy,
        query_first_new,
        query_second_new,
        key_update,
        key_new,
        key_copy,
        key_first_new,
        key_second_new,
    )


def solution(mesh):
    in_specs = (
        P("fs", None),
        P("fs", "tp"),
        P("fs", "tp"),
        P("fs", None),
        P("fs", None),
        P("fs", "tp"),
        P("fs", "tp"),
        P("fs", "tp"),
        P("fs", "tp"),
        P("fs", "tp"),
        P("fs", "tp"),
    )
    out_specs = (
        P("fs", "tp"),
        P("fs", "tp"),
        P(None, "tp"),
        P("fs", "tp"),
        P("fs", "tp"),
        P("fs", "tp"),
        P("fs", "tp"),
        P(None, "tp"),
        P("fs", "tp"),
        P("fs", "tp"),
    )
    return jax.shard_map(
        body, mesh=mesh, in_specs=in_specs, out_specs=out_specs, check_vma=False
    )
```
